32 devices in a mesh: kv: 16 (over z, y, x), tp: 2 (over core).
Axes of the slice: x: 2, y: 2, z: 4, core: 2. Of those that a mesh axis runs over, the one named last changes fastest.
Arguments:
- tokens: bfloat16 [32, 4096], P(None, 'kv'), may hold values from -6 to 6
- norm_gain: bfloat16 [4096], P('kv'), may hold values from 0.099609375 to 1.8984375
- w_query: bfloat16 [4096, 4096], P('kv', 'tp'), may hold values from -0.09375 to 0.09375
- w_key: bfloat16 [4096, 1024], P('kv', 'tp'), may hold values from -0.09375 to 0.09375
- w_value: bfloat16 [4096, 1024], P('kv', 'tp'), may hold values from -0.09375 to 0.09375
- w_forget: bfloat16 [4096, 32], P('kv', 'tp'), may hold values from -0.1875 to 0.1875
- forget_bias: float32 [32], P('tp'), may hold values from -1 to 3
- key_cache: bfloat16 [32, 4096, 1024], P(None, 'kv', 'tp'), may hold values from -1200 to 1200
- value_cache: bfloat16 [32, 4096, 1024], P(None, 'kv', 'tp'), may hold values from -6 to 6
- gate_cache: float32 [32, 32, 4096], P(None, 'tp', 'kv'), may hold values from -515 to 0
- lengths: int32 [32], replicated, may hold values from 1024 to 4095, as said below
- w_out: bfloat16 [4096, 4096], P('tp', 'kv'), may hold values from -0.375 to 0.375
Outputs:
- mixed: bfloat16 [32, 4096], P(None, 'kv')
The draws below stay inside these ranges and needn't reach their ends.
Inputs may be any that keep to these rules, and one draw needn't show every extreme that they name: `lengths`: at least one sequence has the length 4095 in every draw.
All inputs are finite; a program needn't handle non-finite values.
Results may differ from the reference program's by a relative error of at most 0.018.
Values may be sent and summed in bfloat16 or wider, within the bound.
A program may use at most 64 MiB of HBM per device.

```python
import math
import jax
import jax.numpy as jnp
from jax import lax

D = 4096
QUERY_HEADS = 32
KV_HEADS = 8
HEAD_DIM = 128
BATCH_ROWS = 32
P_DEV = 256
CACHE_POSITIONS = 4096
HEADS_DEV = 16
N_TP = 2


def lengths_core(key):
    inner = jax.random.fold_in(key, 11)
    first, second = jax.random.split(inner)
    drawn = jax.random.randint(first, (BATCH_ROWS,), CACHE_POSITIONS // 4, CACHE_POSITIONS)
    longest = jax.random.randint(second, (), 0, BATCH_ROWS)
    drawn = jnp.where(jnp.arange(BATCH_ROWS) == longest, CACHE_POSITIONS - 1, drawn)
    return drawn.astype(jnp.int32)


def draw_lengths(key, part):
    return lengths_core(key)


def draw_gate_cache(key, part):
    seq_len = lengths_core(key)
    key_rows = jax.random.split(jax.random.fold_in(key, 23), 5)
    fast_share = 0.5
    fast = jax.random.uniform(key_rows[0], (QUERY_HEADS,)) < fast_share
    rates = jnp.where(fast, 1.0 / 40.0, 1.0 / CACHE_POSITIONS).astype(jnp.float32)
    block_rates = jnp.exp(jax.random.uniform(key_rows[1], (BATCH_ROWS, 1, CACHE_POSITIONS // P_DEV), jnp.float32, -math.log(2.0), math.log(2.0)))
    block_rates = jnp.repeat(block_rates, P_DEV, axis=2)
    rough = jnp.exp(jax.random.uniform(key_rows[2], (BATCH_ROWS, QUERY_HEADS, CACHE_POSITIONS), jnp.float32, -math.log(2.0), math.log(2.0)))
    gate_logarithms = -rates[None, :, None] * block_rates * rough
    segment_start = jax.random.randint(key_rows[3], (BATCH_ROWS, 3), 0, CACHE_POSITIONS)
    segment_length = jnp.log(jax.random.uniform(key_rows[4], (BATCH_ROWS, 3), jnp.float32, 0.5, 0.8))
    write_position = jnp.arange(CACHE_POSITIONS)
    position_indicator = (write_position[None, None, :] == segment_start[:, :, None]).astype(jnp.float32)
    segment_count = jnp.sum(position_indicator * segment_length[:, :, None], axis=1)
    gate_logarithms = gate_logarithms + segment_count[:, None, :]
    inside = write_position[None, :] < seq_len[:, None]
    gate_logarithms = jnp.where(inside[:, None, :], gate_logarithms, 0.0)
    suffix = jnp.cumsum(gate_logarithms[..., ::-1], axis=-1)[..., ::-1] - gate_logarithms
    return suffix.astype(jnp.float32)


def draw_key_cache(key, part):
    key_rows = jax.random.split(jax.random.fold_in(key, 37), 1)
    base = jnp.clip(jax.random.normal(key_rows[0], (BATCH_ROWS, CACHE_POSITIONS, KV_HEADS * HEAD_DIM), jnp.float32), -6.0, 6.0)
    return base.astype(jnp.bfloat16)


def steps_of(own_key, shape, pieces, low, top_value):
    loudness, own = 1.0, jax.random.fold_in(own_key, 6)
    for dim, blocks in pieces:
        steps = jnp.exp(jax.random.uniform(jax.random.fold_in(own, dim), (blocks,), jnp.float32, low / len(pieces), top_value / len(pieces)))
        loudness = loudness * jnp.repeat(steps, shape[dim] // blocks).reshape([-1 if axis == dim else 1 for axis in range(len(shape))])
    return loudness


def centred(rng, extent, spread, limit, cuts=(), kind=jnp.bfloat16):
    factor_of = steps_of(rng, extent, cuts, -0.22, 0.18) if cuts else 1.0
    values = jax.random.normal(rng, extent, jnp.float32) * spread * factor_of
    return jnp.minimum(jnp.maximum(values, -limit), limit).astype(kind)


def setup_inputs(seed: int = 0) -> dict:
    seeds = jax.random.split(jax.random.key(seed), 13)
    tokens = centred(seeds[0], (BATCH_ROWS, D), 1.0, 6.0, ((1, 16),))
    norm_gain = jnp.clip(1.0 + 0.18 * jax.random.normal(seeds[1], (D,), jnp.float32), 0.099609375, 1.8984375).astype(jnp.bfloat16)
    w_query = centred(seeds[2], (D, QUERY_HEADS * HEAD_DIM), D ** -0.5, 0.09375, ((0, 16), (1, 2)))
    w_key = centred(seeds[3], (D, KV_HEADS * HEAD_DIM), D ** -0.5, 0.09375, ((0, 16), (1, 2)))
    w_value = centred(seeds[4], (D, KV_HEADS * HEAD_DIM), D ** -0.5, 0.09375, ((0, 16), (1, 2)))
    w_forget = centred(seeds[5], (D, QUERY_HEADS), (D // 4) ** -0.5, 0.1875, ((0, 16), (1, 2)))
    forget_bias = jnp.clip(-1.0 + 4.0 * jax.random.uniform(seeds[6], (QUERY_HEADS,), jnp.float32) ** steps_of(seeds[6], (QUERY_HEADS,), ((0, 2),), -0.2, 0.2), -1.0, 3.0)
    key_cache = draw_key_cache(jax.random.fold_in(seeds[12], 71), 0)
    value_cache = centred(seeds[8], (BATCH_ROWS, CACHE_POSITIONS, KV_HEADS * HEAD_DIM), 1.0, 6.0, ((1, 16), (2, 2)))
    gate_cache = draw_gate_cache(jax.random.fold_in(seeds[12], 71), 0)
    lengths = draw_lengths(jax.random.fold_in(seeds[12], 71), 0)
    w_out = centred(seeds[11], (QUERY_HEADS * HEAD_DIM, D), (QUERY_HEADS * HEAD_DIM // 16) ** -0.5, 0.375, ((0, 2), (1, 16)))
    return {"tokens": tokens, "norm_gain": norm_gain, "w_query": w_query, "w_key": w_key, "w_value": w_value, "w_forget": w_forget, "forget_bias": forget_bias, "key_cache": key_cache, "value_cache": value_cache, "gate_cache": gate_cache, "lengths": lengths, "w_out": w_out}


EPSILON = 1e-06
NEGATIVE = -1e+30

def reference(tokens, norm_gain, w_query, w_key, w_value, w_forget, forget_bias, key_cache, value_cache, gate_cache, lengths, w_out):
    batch_rows = tokens.shape[0]
    groups = QUERY_HEADS // KV_HEADS
    score_scaling = HEAD_DIM ** (-0.5)
    tokens_f = tokens.astype(jnp.float32)
    inverse = lax.rsqrt(lax.optimization_barrier(jnp.mean(tokens_f * tokens_f, axis=1)) + EPSILON)
    scaled = (tokens_f * norm_gain.astype(jnp.float32)[None, :]).astype(jnp.bfloat16)
    query_rows = (jnp.dot(scaled, w_query, preferred_element_type=jnp.float32) * inverse[:, None]).astype(jnp.bfloat16)
    fresh_key = (jnp.dot(scaled, w_key, preferred_element_type=jnp.float32) * inverse[:, None]).astype(jnp.bfloat16)
    new_value = (jnp.dot(scaled, w_value, preferred_element_type=jnp.float32) * inverse[:, None]).astype(jnp.bfloat16)
    forget = jnp.dot(scaled, w_forget, preferred_element_type=jnp.float32) * inverse[:, None] + forget_bias[None, :]
    forget_logarithm = jax.nn.log_sigmoid(forget)
    query_float = query_rows.astype(jnp.float32).reshape(batch_rows, KV_HEADS, groups, HEAD_DIM)
    blocks = CACHE_POSITIONS // P_DEV

    def one_block(index):
        start = (index * P_DEV).astype(jnp.int32)
        key_rows = lax.dynamic_slice_in_dim(key_cache, start, P_DEV, 1).astype(jnp.float32).reshape(batch_rows, P_DEV, KV_HEADS, HEAD_DIM)
        values = lax.dynamic_slice_in_dim(value_cache, start, P_DEV, 1).astype(jnp.float32).reshape(batch_rows, P_DEV, KV_HEADS, HEAD_DIM)
        gates = lax.dynamic_slice_in_dim(gate_cache, start, P_DEV, 2)
        scores = jnp.einsum('bkgd,bpkd->bkgp', query_float, key_rows).reshape(batch_rows, QUERY_HEADS, P_DEV)
        scores = scores * score_scaling + gates
        position = start + jnp.arange(P_DEV, dtype=jnp.int32)
        valid = position[None, None, :] < lengths[:, None, None]
        scores = jnp.where(valid, scores, NEGATIVE)
        block_max = lax.optimization_barrier(jnp.max(scores, axis=2))
        weights = jnp.where(valid, jnp.exp(scores - block_max[..., None]), 0.0)
        block_sum = lax.optimization_barrier(jnp.sum(weights, axis=2))
        weights_low = weights.astype(jnp.bfloat16).astype(jnp.float32).reshape(batch_rows, KV_HEADS, groups, P_DEV)
        block_values = jnp.einsum('bkgp,bpkd->bkgd', weights_low, values).reshape(batch_rows, QUERY_HEADS, HEAD_DIM)
        return (block_max, block_sum, block_values)
    block_max, block_sum, block_values = lax.map(one_block, jnp.arange(blocks, dtype=jnp.int32))
    key_float = fresh_key.astype(jnp.float32).reshape(batch_rows, KV_HEADS, HEAD_DIM)
    self_token = jnp.einsum('cptj,cpj->cpt', query_float, key_float).reshape(batch_rows, QUERY_HEADS) * score_scaling - forget_logarithm
    top = jnp.maximum(lax.optimization_barrier(jnp.max(block_max, axis=0)), self_token)
    factor = jnp.exp(block_max - top[None])
    own_weight = jnp.exp(self_token - top)
    total = lax.optimization_barrier(jnp.sum(block_sum * factor, axis=0)) + own_weight
    own_values = jnp.repeat(new_value.astype(jnp.float32).reshape(batch_rows, KV_HEADS, HEAD_DIM), groups, axis=1)
    summed = lax.optimization_barrier(jnp.sum(block_values * factor[..., None], axis=0)) + own_weight[..., None] * own_values
    attended = (summed / total[..., None]).astype(jnp.bfloat16).reshape(batch_rows, N_TP, HEADS_DEV * HEAD_DIM)
    weight_blocks = w_out.astype(jnp.float32).reshape(N_TP, HEADS_DEV * HEAD_DIM, D)
    partial_value = jnp.einsum('bgi,gid->bgd', attended.astype(jnp.float32), weight_blocks)
    partial_value = lax.optimization_barrier(partial_value.astype(jnp.bfloat16)).astype(jnp.float32)
    return lax.optimization_barrier(jnp.sum(partial_value, axis=1)).astype(jnp.bfloat16)
```

```python
import functools

import jax
import jax.numpy as jnp
from jax import lax
from jax.experimental import pallas as pl
from jax.experimental.pallas import tpu as pltpu
from jax.sharding import PartitionSpec as P

HEAD_DIM = 128
EPSILON = 1e-06
NEGATIVE = -1e30
ROWS = 8
PARTS = 8
F32 = jnp.float32
BF16 = jnp.bfloat16


def iota(shape, dim):
    return lax.broadcasted_iota(jnp.int32, shape, dim)


def one_hot(condition):
    return jnp.where(condition, 1.0, 0.0).astype(BF16)


def dot(a, b):
    return jnp.dot(a, b, preferred_element_type=F32)


def round_low(x):
    return x.astype(BF16).astype(F32)


def split3(x):
    high = round_low(x)
    rest = x - high
    mid = round_low(rest)
    return high, mid, round_low(rest - mid)


def kernel(
    n, tp, heads, kv_count, batch, span, width,
    tokens_ref, gain_ref, bias_ref, lengths_ref,
    wq_hbm, wk_hbm, wv_hbm, wf_ref, k_hbm, v_hbm, gate_hbm, wo_hbm,
    out_ref,
    wq, wk, wv, kbuf, vbuf, gate, wo,
    send1, recv1, qbuf, send2, recv2, stat, att, pair,
    wsem, ksem, vsem, gsem,
    s1, r1, s2, r2, s3, r3, s4, r4, s5, r5,
):
    me = lax.axis_index("kv")
    my_tp = lax.axis_index("tp")
    groups = heads // kv_count
    row_groups = batch // ROWS
    units = row_groups * kv_count
    stride = n // units
    qcols = groups * HEAD_DIM
    unit_rows = groups * ROWS
    scale = HEAD_DIM ** (-0.5)
    my_unit = me // stride
    my_r = my_unit // kv_count
    my_g = my_unit % kv_count
    is_owner = (me % stride) == 0

    def owner_only(body):
        if stride == 1:
            body()
        else:
            pl.when(is_owner)(body)

    barrier = pltpu.get_barrier_semaphore()

    def greet(k, carry):
        pl.semaphore_signal(
            barrier, inc=1, device_id={"kv": lax.rem(me + k, n)},
            device_id_type=pl.DeviceIdType.MESH,
        )
        return carry

    lax.fori_loop(1, n, greet, 0)
    for k in range(1, tp):
        pl.semaphore_signal(
            barrier, inc=1, device_id={"tp": lax.rem(my_tp + k, tp)},
            device_id_type=pl.DeviceIdType.MESH,
        )

    w_copies = [
        pltpu.make_async_copy(src, dst, wsem.at[i])
        for i, (src, dst) in enumerate(((wq_hbm, wq), (wk_hbm, wk), (wv_hbm, wv)))
    ]
    wo_copy = pltpu.make_async_copy(wo_hbm, wo, wsem.at[3])
    gate_copy = pltpu.make_async_copy(gate_hbm, gate, gsem)
    for c in w_copies:
        c.start()

    def cache_copy(hbm, buf, sems, r):
        rows = pl.ds(pl.multiple_of(r * ROWS, ROWS), ROWS)
        return pltpu.make_async_copy(hbm.at[rows], buf.at[rows], sems.at[r])

    tokens_f = tokens_ref[...].astype(F32)
    squares = jnp.sum(tokens_f * tokens_f, axis=1, keepdims=True)
    scaled = (tokens_f * gain_ref[...].astype(F32)).astype(BF16)
    forget = dot(scaled, wf_ref[...])
    lane = iota((batch, HEAD_DIM), 1)
    fh = round_low(forget)
    fl = forget - fh
    place_r = iota((heads, HEAD_DIM), 0)
    place_c = iota((heads, HEAD_DIM), 1)
    sh, sm, sl = split3(squares)
    extra = (
        dot(fh.astype(BF16), one_hot(place_c == place_r))
        + dot(fl.astype(BF16), one_hot(place_c == place_r + heads))
        + jnp.where(lane == 2 * heads, sh, 0.0)
        + jnp.where(lane == 2 * heads + 1, sm, 0.0)
        + jnp.where(lane == 2 * heads + 2, sl, 0.0)
    )
    for c in w_copies:
        c.wait()
    for k in range(row_groups):
        r = lax.rem(my_r + k, row_groups)
        cache_copy(k_hbm, kbuf, ksem, r).start()
        if k == 0:
            gate_copy.start()
        cache_copy(v_hbm, vbuf, vsem, r).start()
    wo_copy.start()

    for g in range(kv_count):
        qg = dot(scaled, wq[:, g * qcols:(g + 1) * qcols])
        kg = dot(scaled, wk[:, g * HEAD_DIM:(g + 1) * HEAD_DIM])
        vg = dot(scaled, wv[:, g * HEAD_DIM:(g + 1) * HEAD_DIM])
        for r in range(row_groups):
            at = slice(r * ROWS, (r + 1) * ROWS)
            u = r * kv_count + g
            send1[u, :, 0:qcols] = qg[at].astype(BF16)
            send1[u, :, qcols:qcols + HEAD_DIM] = kg[at].astype(BF16)
            send1[u, :, qcols + HEAD_DIM:qcols + 2 * HEAD_DIM] = vg[at].astype(BF16)
            send1[u, :, qcols + 2 * HEAD_DIM:qcols + 3 * HEAD_DIM] = extra[at].astype(BF16)

    pl.semaphore_wait(barrier, n - 1 + tp - 1)

    def rs1(u):
        return pltpu.make_async_remote_copy(
            src_ref=send1.at[u], dst_ref=recv1.at[me], send_sem=s1.at[u],
            recv_sem=r1.at[me], device_id={"kv": u * stride},
            device_id_type=pl.DeviceIdType.MESH,
        )

    def rs1_from(d):
        return pltpu.make_async_remote_copy(
            src_ref=send1.at[0], dst_ref=recv1.at[d], send_sem=s1.at[0],
            recv_sem=r1.at[d], device_id={"kv": me}, device_id_type=pl.DeviceIdType.MESH,
        )

    def start_rs1(k, carry):
        u = lax.rem(my_unit + k, units)

        @pl.when(u * stride != me)
        def _():
            rs1(u).start()
        return carry

    lax.fori_loop(0, units, start_rs1, 0)

    def ag1(u, d):
        return pltpu.make_async_remote_copy(
            src_ref=qbuf.at[u], dst_ref=qbuf.at[u], send_sem=s2.at[d],
            recv_sem=r2.at[u], device_id={"kv": d}, device_id_type=pl.DeviceIdType.MESH,
        )

    own_parts = {}

    def project():
        total0 = send1[my_unit].astype(F32)

        def add(k, acc):
            d = lax.rem(me + k, n)
            rs1_from(d).wait_recv()
            return acc + recv1[d].astype(F32)

        sums = lax.fori_loop(1, n, add, total0)
        fs = sums[:, qcols + 2 * HEAD_DIM:]
        fl8 = iota((ROWS, HEAD_DIM), 1)

        def pick(mask):
            return jnp.sum(jnp.where(mask, fs, 0.0), axis=1, keepdims=True)

        square = pick((fl8 >= 2 * heads) & (fl8 <= 2 * heads + 2))
        inverse = lax.rsqrt(square / width + EPSILON)
        query = round_low(sums[:, :qcols] * inverse)
        by_head = [query[:, h * HEAD_DIM:(h + 1) * HEAD_DIM] for h in range(groups)]
        qbuf[my_unit] = jnp.concatenate(by_head, axis=0).astype(BF16)

        def send(k, carry):
            ag1(my_unit, lax.rem(me + k, n)).start()
            return carry

        lax.fori_loop(1, n, send, 0)
        new_key = round_low(sums[:, qcols:qcols + HEAD_DIM] * inverse)
        new_value = round_low(sums[:, qcols + HEAD_DIM:qcols + 2 * HEAD_DIM] * inverse)
        owns = []
        for h in range(groups):
            head = my_g * groups + h
            x = pick((fl8 == head) | (fl8 == head + heads)) * inverse + bias_ref[head]
            softplus = jnp.maximum(-x, 0.0) + jnp.log1p(jnp.exp(-jnp.abs(x)))
            score = jnp.sum(by_head[h] * new_key, axis=1, keepdims=True) * scale + softplus
            owns.append(jnp.broadcast_to(score, (ROWS, HEAD_DIM)))
        own_parts["score"] = jnp.concatenate(owns, axis=1)
        own_parts["value"] = new_value
        pair_own[0] = own_parts["score"]
        pair_own[1] = jnp.concatenate([new_value] * groups, axis=1)

    pair_own = stat["own"]
    owner_only(project)

    gate_copy.wait()
    m_rows = ROWS * heads

    def rs2(u):
        return pltpu.make_async_remote_copy(
            src_ref=send2.at[u], dst_ref=recv2.at[me], send_sem=s3.at[u],
            recv_sem=r3.at[me], device_id={"kv": u * stride},
            device_id_type=pl.DeviceIdType.MESH,
        )

    def rs2_from(d):
        return pltpu.make_async_remote_copy(
            src_ref=send2.at[0], dst_ref=recv2.at[d], send_sem=s3.at[0],
            recv_sem=r3.at[d], device_id={"kv": me}, device_id_type=pl.DeviceIdType.MESH,
        )

    def ag1_from(u):
        return ag1(u, me)

    def attend(step, carry):
        r = lax.rem(my_r + step, row_groups)
        si = iota((m_rows, unit_rows), 0)
        sj = iota((m_rows, unit_rows), 1)
        blocks = []
        for g in range(kv_count):
            u = r * kv_count + g

            @pl.when(u * stride != me)
            def _():
                ag1_from(u).wait_recv()
            source = (si % heads - g * groups) * ROWS + si // heads
            inside = (si % heads) // groups == g
            blocks.append(dot(one_hot(inside & (sj == source)), qbuf[u]).astype(BF16))
        queries = jnp.concatenate(blocks, axis=1)
        cache_copy(k_hbm, kbuf, ksem, r).wait()
        position = me * span + iota((heads, span), 1)
        scores, valids = [], []
        for b in range(ROWS):
            row = r * ROWS + b
            s = lax.dot_general(
                queries[b * heads:(b + 1) * heads], kbuf[row],
                (((1,), (1,)), ((), ())), preferred_element_type=F32,
            )
            s = s * scale + gate[row]
            valid = position < lengths_ref[row]
            scores.append(jnp.where(valid, s, NEGATIVE))
            valids.append(jnp.where(valid, 1.0, 0.0))
        score = jnp.concatenate(scores, axis=0)
        kept = jnp.concatenate(valids, axis=0) > 0.0
        top = jnp.max(score, axis=1, keepdims=True)
        weight = jnp.where(kept, jnp.exp(score - top), 0.0)
        total = jnp.sum(weight, axis=1, keepdims=True)
        low = weight.astype(BF16)
        cache_copy(v_hbm, vbuf, vsem, r).wait()
        values = []
        head_group = iota((heads, HEAD_DIM), 0) // groups
        for b in range(ROWS):
            full = dot(low[b * heads:(b + 1) * heads], vbuf[r * ROWS + b])
            mine = full[:, :HEAD_DIM]
            for g in range(1, kv_count):
                mine = jnp.where(head_group == g, full[:, g * HEAD_DIM:(g + 1) * HEAD_DIM], mine)
            values.append(mine.astype(BF16))
        value = jnp.concatenate(values, axis=0)

        li = iota((m_rows, HEAD_DIM), 0)
        ll = iota((m_rows, HEAD_DIM), 1)
        here = ll // PARTS == li % groups

        def spread(x):
            a, b, c = split3(x)
            part = ll % PARTS
            picked = jnp.where(part == 0, a, jnp.where(part == 1, b, jnp.where(part == 2, c, 0.0)))
            return jnp.where(here, picked, 0.0).astype(BF16)

        ti = iota((m_rows, m_rows), 0)
        tj = iota((m_rows, m_rows), 1)
        moved = dot(one_hot(tj == (ti % ROWS) * heads + ti // ROWS), value).astype(BF16)
        wi = iota((kv_count * ROWS, m_rows), 0)
        wj = iota((kv_count * ROWS, m_rows), 1)
        gather = one_hot((wj // heads == wi % ROWS) & ((wj % heads) // groups == wi // ROWS))
        tops = dot(gather, spread(top))
        totals = dot(gather, spread(total))
        for g in range(kv_count):
            u = r * kv_count + g
            at = slice(g * ROWS, (g + 1) * ROWS)
            send2[u, 0:unit_rows] = moved[g * unit_rows:(g + 1) * unit_rows]
            send2[u, unit_rows:unit_rows + 2 * ROWS] = jnp.concatenate(
                [tops[at], totals[at]], axis=0
            ).astype(BF16)

            @pl.when(u * stride != me)
            def _():
                rs2(u).start()
        return carry

    lax.fori_loop(0, row_groups, attend, 0)

    def ag2(u, d):
        return pltpu.make_async_remote_copy(
            src_ref=att.at[u], dst_ref=att.at[u], send_sem=s4.at[d],
            recv_sem=r4.at[u], device_id={"kv": d}, device_id_type=pl.DeviceIdType.MESH,
        )

    def slot(u):
        return lax.rem(u, kv_count) * row_groups + u // kv_count

    def join():
        recv2[me] = send2[my_unit]

        def arrived(k, carry):
            rs2_from(lax.rem(me + k, n)).wait_recv()
            return carry

        lax.fori_loop(1, n, arrived, 0)
        ei = iota((HEAD_DIM, qcols), 0)
        ej = iota((HEAD_DIM, qcols), 1)
        widen = one_hot((ei // PARTS == ej // HEAD_DIM) & (ei % PARTS < 3))
        packed = recv2[:, unit_rows:unit_rows + 2 * ROWS, :].reshape(n * 2 * ROWS, HEAD_DIM)
        stat["all"][...] = dot(packed, widen).reshape(n, 2 * ROWS, qcols)
        own = pair_own[0]

        def highest(d, top):
            return jnp.maximum(top, stat["all"][d, 0:ROWS])

        top = lax.fori_loop(0, n, highest, own, unroll=4)

        def gather(d, carry):
            total, acc = carry
            factor = jnp.exp(stat["all"][d, 0:ROWS] - top)
            piece = recv2[d, 0:unit_rows].astype(F32)
            piece = jnp.concatenate(
                [piece[h * ROWS:(h + 1) * ROWS] for h in range(groups)], axis=1
            )
            return total + stat["all"][d, ROWS:2 * ROWS] * factor, acc + piece * factor

        own_weight = jnp.exp(own - top)
        total, acc = lax.fori_loop(
            0, n, gather, (own_weight, own_weight * pair_own[1]), unroll=4
        )
        att[slot(my_unit)] = (acc / total).astype(BF16)

        def send(k, carry):
            ag2(slot(my_unit), lax.rem(me + k, n)).start()
            return carry

        lax.fori_loop(1, n, send, 0)

    owner_only(join)

    wo_copy.wait()
    part = None
    for g in range(kv_count):
        for r in range(row_groups):
            @pl.when((r * kv_count + g) * stride != me)
            def _():
                ag2(g * row_groups + r, me).wait_recv()
        rows = att[g * row_groups:(g + 1) * row_groups].astype(F32).reshape(batch, qcols).astype(BF16)
        term = dot(rows, wo[g * qcols:(g + 1) * qcols, :])
        part = term if part is None else part + term

    pair[my_tp] = part.astype(BF16)
    exchanges = []
    for k in range(1, tp):
        c = pltpu.make_async_remote_copy(
            src_ref=pair.at[my_tp], dst_ref=pair.at[my_tp], send_sem=s5.at[k],
            recv_sem=r5.at[my_tp], device_id={"tp": lax.rem(my_tp + k, tp)},
            device_id_type=pl.DeviceIdType.MESH,
        )
        c.start()
        exchanges.append(c)
    for k in range(1, tp):
        other = lax.rem(my_tp + k, tp)
        pltpu.make_async_remote_copy(
            src_ref=pair.at[other], dst_ref=pair.at[other], send_sem=s5.at[k],
            recv_sem=r5.at[other], device_id={"tp": my_tp},
            device_id_type=pl.DeviceIdType.MESH,
        ).wait_recv()
    summed = pair[0].astype(F32)
    for k in range(1, tp):
        summed = summed + pair[k].astype(F32)
    out_ref[...] = summed

    def drain_units(u, carry):
        @pl.when(u * stride != me)
        def _():
            rs1(u).wait_send()
            rs2(u).wait_send()
        return carry

    lax.fori_loop(0, units, drain_units, 0)

    def drain_owner():
        def drain(k, carry):
            d = lax.rem(me + k, n)
            ag1(my_unit, d).wait_send()
            ag2(slot(my_unit), d).wait_send()
            return carry

        lax.fori_loop(1, n, drain, 0)

    owner_only(drain_owner)
    for c in exchanges:
        c.wait_send()


def solution(mesh):
    n, tp = mesh.shape["kv"], mesh.shape["tp"]

    def local(
        tokens, norm_gain, w_query, w_key, w_value, w_forget, forget_bias,
        key_cache, value_cache, gate_cache, lengths, w_out,
    ):
        batch, depth = tokens.shape
        heads, span = gate_cache.shape[1], gate_cache.shape[2]
        kv_count = key_cache.shape[2] // HEAD_DIM
        groups = heads // kv_count
        qcols = groups * HEAD_DIM
        units = batch // ROWS * kv_count
        assert n % units == 0
        out_cols = w_out.shape[1]
        vmem = pl.BlockSpec(memory_space=pltpu.VMEM)
        smem = pl.BlockSpec(memory_space=pltpu.SMEM)
        hbm = pl.BlockSpec(memory_space=pl.ANY)
        dma = pltpu.SemaphoreType.DMA
        body = functools.partial(
            kernel, n, tp, heads, kv_count, batch, span, float(n * depth)
        )
        summed = pl.pallas_call(
            body,
            out_shape=jax.ShapeDtypeStruct((batch, out_cols), F32),
            in_specs=[vmem, vmem, smem, smem, hbm, hbm, hbm, vmem, hbm, hbm, hbm, hbm],
            out_specs=vmem,
            scratch_shapes=[
                pltpu.VMEM(w_query.shape, BF16),
                pltpu.VMEM(w_key.shape, BF16),
                pltpu.VMEM(w_value.shape, BF16),
                pltpu.VMEM(key_cache.shape, BF16),
                pltpu.VMEM(value_cache.shape, BF16),
                pltpu.VMEM(gate_cache.shape, F32),
                pltpu.VMEM(w_out.shape, BF16),
                pltpu.VMEM((units, ROWS, qcols + 3 * HEAD_DIM), BF16),
                pltpu.VMEM((n, ROWS, qcols + 3 * HEAD_DIM), BF16),
                pltpu.VMEM((units, groups * ROWS, HEAD_DIM), BF16),
                pltpu.VMEM((units, (groups + 2) * ROWS, HEAD_DIM), BF16),
                pltpu.VMEM((n, (groups + 2) * ROWS, HEAD_DIM), BF16),
                {
                    "all": pltpu.VMEM((n, 2 * ROWS, qcols), F32),
                    "own": pltpu.VMEM((2, ROWS, qcols), F32),
                },
                pltpu.VMEM((units, ROWS, qcols), BF16),
                pltpu.VMEM((tp, batch, out_cols), BF16),
                dma((4,)), dma((batch // ROWS,)), dma((batch // ROWS,)), dma,
                dma((units,)), dma((n,)), dma((n,)), dma((units,)),
                dma((units,)), dma((n,)), dma((n,)), dma((units,)),
                dma((tp,)), dma((tp,)),
            ],
            compiler_params=pltpu.CompilerParams(
                collective_id=0, has_side_effects=True, vmem_limit_bytes=48 * 2**20
            ),
        )(
            tokens, norm_gain.reshape(1, depth), forget_bias, lengths,
            w_query, w_key, w_value, w_forget, key_cache, value_cache, gate_cache, w_out,
        )
        return summed.astype(BF16)

    in_specs = (
        P(None, "kv"), P("kv"), P("kv", "tp"), P("kv", "tp"), P("kv", "tp"),
        P("kv", "tp"), P("tp"), P(None, "kv", "tp"), P(None, "kv", "tp"),
        P(None, "tp", "kv"), P(), P("tp", "kv"),
    )
    return jax.shard_map(
        local, mesh=mesh, in_specs=in_specs, out_specs=P(None, "kv"), check_vma=False
    )
```
